32 devices in a mesh: ep: 8 (over z, core), tp: 4 (over y, x).
Axes of the slice: x: 2, y: 2, z: 4, core: 2. Of those that a mesh axis runs over, the one named last changes fastest.
Arguments:
- outer_gate: bfloat16 [1024, 2048], P('ep', 'tp'), may hold values from -6 to 6
- inner_gate: bfloat16 [1024, 2048], P('ep', 'tp'), may hold values from -6 to 6
- conv_value: bfloat16 [1024, 2048], P('ep', 'tp'), may hold values from -6 to 6
- conv_taps: bfloat16 [3, 2048], P(None, 'tp'), may hold values from -3.5 to 3.5
- mix_out: bfloat16 [2048, 2048], P(None, 'tp')
- gain_mixer: bfloat16 [2048], P('tp'), may hold values from 0.099609375 to 1.8984375
- bias_mixer: bfloat16 [2048], P('tp'), may hold values from -3 to 3
- moe_input: bfloat16 [1024, 2048], P('ep'), may hold values from -6 to 6
- route_ids: int32 [1024, 4], P('ep'), may hold values from 0 to 7, all different within a row; in each aligned block of 128 rows (0 to 127, 128 to 255, ...) at most 96 rows name the same one
- route_weights: float32 [1024, 4], P('ep'), may hold values from 0.1 to 1.2
- expert_gate: bfloat16 [8, 2048, 2048], P('ep', None, 'tp'), may hold values from -0.125 to 0.125
- expert_up: bfloat16 [8, 2048, 2048], P('ep', None, 'tp'), may hold values from -0.125 to 0.125
- expert_down: bfloat16 [8, 2048, 2048], P('ep', None, 'tp')
- shared_gate: bfloat16 [2048, 2048], P(None, 'tp'), may hold values from -0.125 to 0.125
- shared_up: bfloat16 [2048, 2048], P(None, 'tp'), may hold values from -0.125 to 0.125
- shared_down: bfloat16 [2048, 2048], P(None, 'tp')
- gain_experts: bfloat16 [2048], P('tp'), may hold values from 0.099609375 to 1.8984375
- bias_experts: bfloat16 [2048], P('tp'), may hold values from -3 to 3
Outputs:
- out_mixer: bfloat16 [1024, 2048], P('ep', 'tp')
- out_experts: bfloat16 [1024, 2048], P('ep', 'tp')
The draws below stay inside these ranges and needn't reach their ends.
Inputs may be any that keep to these rules, and one draw needn't show every extreme that they name: `route_ids`: each row names 4 different experts. Among the rows of one index of ep (aligned blocks of 128 rows) no expert is named more than 96 times, a bound that some block reaches.
All inputs are finite; a program needn't handle non-finite values.
Results may differ from the reference program's by a relative error of at most 0.0055.
Values may be sent and summed in bfloat16 or wider, within the bound.
A program may use at most 64 MiB of HBM per device.

```python
import math
import jax
import jax.numpy as jnp
import numpy as np
from jax import lax

D = 2048
EFF = 2048
SFF = 2048
KERNEL = 3
TOPK = 4
ROWS = 128
TOKENS = 1024
EXPERTS = 8
CAP = 96
SEQ_LEN = 1024
N_EP = 8


def column_scales(key, width):
    place = jnp.arange(width, dtype=jnp.float32) / width
    rough = jax.random.uniform(jax.random.fold_in(key, 7), (width,), jnp.float32, 0.5, 2.0)
    return jnp.exp(jnp.log(10.0) * place) * rough


def draw_mix_out(key, part):
    values = jax.random.normal(jax.random.fold_in(key, 11), (D, D), jnp.float32) * D ** (-0.5)
    return (values * column_scales(key, D)[None, :]).astype(jnp.bfloat16)


def draw_expert_down(key, part):
    values = jax.random.normal(jax.random.fold_in(key, 13), (EXPERTS, EFF, D), jnp.float32) * EFF ** (-0.5)
    return (values * column_scales(key, D)[None, None, :]).astype(jnp.bfloat16)


def draw_shared_down(key, part):
    values = jax.random.normal(jax.random.fold_in(key, 17), (SFF, D), jnp.float32) * SFF ** (-0.5)
    return (values * column_scales(key, D)[None, :]).astype(jnp.bfloat16)


def level_of(rng, shape, shards, smallest, top_value):
    factor_of, own = 1.0, jax.random.fold_in(rng, 6)
    for position, parts in shards:
        steps = jnp.exp(jax.random.uniform(jax.random.fold_in(own, position), (parts,), jnp.float32, smallest / len(shards), top_value / len(shards)))
        factor_of = factor_of * jnp.repeat(steps, shape[position] // parts).reshape([-1 if axis == position else 1 for axis in range(len(shape))])
    return factor_of


def assign_block(own_key, own, number, rows, count, top, reach, skew):
    order = jax.random.permutation(own_key, count)
    heavy_load, common = shares(count, rows * top, reach, skew, True), shares(count, rows * top, reach, skew, False)
    places = jnp.arange(count)

    def named(lengths, turn):
        used = int((lengths > 0).sum())
        fixed = max(1, used // 4)
        passed = fixed + (places - fixed + turn * (used - fixed)) % max(1, count - fixed)
        return jnp.zeros((count,), jnp.int32).at[order[jnp.where(places < fixed, places, passed)]].set(jnp.asarray(lengths, jnp.int32))

    lengths = jnp.where(number % 4 == 0, named(heavy_load, number // 4), named(common, number - number // 4 - 1))
    mixed = jax.random.permutation(jax.random.fold_in(own, 3), count)
    donor, sink = mixed[0:count // 2 * 2:2], mixed[1:count // 2 * 2:2]
    room = jnp.minimum(lengths[donor] - 1, reach - lengths[sink]) // 2
    room = jnp.where((donor == order[0]) | (sink == order[0]) | (lengths[sink] == 0), 0, jnp.maximum(room, 0))
    passed = jax.random.randint(jax.random.fold_in(own, 4), (count // 2,), 0, 1 << 20) % (room + 1)
    lengths = lengths.at[donor].add(-passed).at[sink].add(passed)
    items = jnp.searchsorted(jnp.cumsum(lengths), jnp.arange(rows * top), side="right").astype(jnp.int32)
    grid = items.reshape(top, rows).T
    grid = grid[jax.random.permutation(jax.random.fold_in(own, 1), rows)]
    turn = jax.random.randint(jax.random.fold_in(own, 2), (rows, 1), 0, top)
    return jnp.take_along_axis(grid, (jnp.arange(top)[None, :] + turn) % top, axis=1)


def shares(number_of, total, reach, slope, full):
    portions = [(1 << 20) // math.isqrt(rank ** slope) + 1 for rank in range(1, number_of + 1)]
    largest = reach if full else min(reach, max(-(-total // number_of), total * portions[0] // sum(portions)))
    least = 1 if total - largest >= number_of - 1 else 0
    given, surplus = [largest] + [least] * (number_of - 1), total - largest - least * (number_of - 1)
    while surplus > 0:
        candidates = [i for i in range(1, number_of) if given[i] < largest] or [i for i in range(1, number_of) if given[i] < reach]
        mass, budget = sum([portions[i] for i in candidates]), surplus
        for i in candidates:
            addition = min(reach - given[i], max(1, budget * portions[i] // mass), surplus)
            given[i] = given[i] + addition
            surplus = surplus - addition
    return np.array(given)


def gaussian(own_key, shape, scale, bound, cuts=(), kind=jnp.bfloat16):
    drawn = jax.random.normal(own_key, shape, jnp.float32) * scale
    if len(cuts) > 0:
        drawn = level_of(own_key, shape, cuts, -0.22, 0.18) * drawn
    return jnp.clip(drawn, min=-bound, max=bound).astype(kind)


def setup_inputs(seed: int = 0) -> dict:
    key_list = jax.random.split(jax.random.key(seed), 19)
    outer_gate = gaussian(key_list[0], (TOKENS, D), 1.0, 6.0, ((0, 8), (1, 4)))
    inner_gate = gaussian(key_list[1], (TOKENS, D), 1.0, 6.0, ((0, 8), (1, 4)))
    conv_value = gaussian(key_list[2], (TOKENS, D), 1.0, 6.0, ((0, 8), (1, 4)))
    conv_taps = gaussian(key_list[3], (KERNEL, D), KERNEL ** -0.5, 3.5, ((1, 4),))
    mix_out = draw_mix_out(jax.random.fold_in(key_list[18], 71), 0)
    gain_mixer = jnp.clip(1.0 + 0.18 * jax.random.normal(key_list[5], (D,), jnp.float32), 0.099609375, 1.8984375).astype(jnp.bfloat16)
    bias_mixer = gaussian(key_list[6], (D,), 0.5, 3.0, ((0, 4),))
    moe_input = gaussian(key_list[7], (TOKENS, D), 1.0, 6.0, ((0, 8),))
    route_ids_keys = jax.random.split(jax.random.fold_in(key_list[8], 1), TOKENS // ROWS)
    route_ids_turns = jax.random.permutation(jax.random.fold_in(key_list[8], 3), TOKENS // ROWS)
    route_ids = jax.vmap(lambda own, number: assign_block(jax.random.fold_in(key_list[8], 2), own, number, ROWS, EXPERTS, TOPK, CAP, 1))(route_ids_keys, route_ids_turns).reshape((TOKENS, TOPK))
    route_weights = jnp.clip(0.1 + 1.1 * jax.random.uniform(key_list[9], (TOKENS, TOPK), jnp.float32) ** level_of(key_list[9], (TOKENS, TOPK), ((0, 8),), -0.2, 0.2), 0.1, 1.2)
    expert_gate = gaussian(key_list[10], (EXPERTS, D, EFF), D ** -0.5, 0.125, ((0, 8), (2, 4)))
    expert_up = gaussian(key_list[11], (EXPERTS, D, EFF), D ** -0.5, 0.125, ((0, 8), (2, 4)))
    expert_down = draw_expert_down(jax.random.fold_in(key_list[18], 71), 0)
    shared_gate = gaussian(key_list[13], (D, SFF), D ** -0.5, 0.125, ((1, 4),))
    shared_up = gaussian(key_list[14], (D, SFF), D ** -0.5, 0.125, ((1, 4),))
    shared_down = draw_shared_down(jax.random.fold_in(key_list[18], 71), 0)
    gain_experts = jnp.clip(1.0 + 0.18 * jax.random.normal(key_list[16], (D,), jnp.float32), 0.099609375, 1.8984375).astype(jnp.bfloat16)
    bias_experts = gaussian(key_list[17], (D,), 0.5, 3.0, ((0, 4),))
    return {"outer_gate": outer_gate, "inner_gate": inner_gate, "conv_value": conv_value, "conv_taps": conv_taps, "mix_out": mix_out, "gain_mixer": gain_mixer, "bias_mixer": bias_mixer, "moe_input": moe_input, "route_ids": route_ids, "route_weights": route_weights, "expert_gate": expert_gate, "expert_up": expert_up, "expert_down": expert_down, "shared_gate": shared_gate, "shared_up": shared_up, "shared_down": shared_down, "gain_experts": gain_experts, "bias_experts": bias_experts}


def row_norm(values, gain, offset_bias):
    average = lax.optimization_barrier(jnp.mean(values, axis=1, keepdims=True))
    spread = lax.optimization_barrier(jnp.mean(values * values, axis=1, keepdims=True)) - average * average
    scaled = (values - average) * lax.rsqrt(spread + 1e-05)
    return (scaled * gain.astype(jnp.float32) + offset_bias.astype(jnp.float32)).astype(jnp.bfloat16)

def rounded(value):
    narrow = lax.optimization_barrier(value.astype(jnp.bfloat16))
    return narrow.astype(jnp.float32)

def reference(outer_gate, inner_gate, conv_value, conv_taps, mix_out, gain_mixer, bias_mixer, moe_input, route_ids, route_weights, expert_gate, expert_up, expert_down, shared_gate, shared_up, shared_down, gain_experts, bias_experts):
    product = rounded(inner_gate.astype(jnp.float32) * conv_value.astype(jnp.float32))
    length = product.shape[0]
    places = jnp.arange(length, dtype=jnp.int32) % SEQ_LEN
    convolved = jnp.zeros(product.shape, jnp.float32)
    for offset in range(KERNEL):
        delay_rows = KERNEL - 1 - offset
        delayed = jnp.pad(product, ((delay_rows, 0), (0, 0)))[:length]
        kept_mask = (places >= delay_rows).astype(jnp.float32)[:, None]
        convolved = convolved + conv_taps[offset].astype(jnp.float32)[None, :] * delayed * kept_mask
    weighted_in = (outer_gate.astype(jnp.float32) * convolved).astype(jnp.bfloat16)
    mixed = jnp.dot(weighted_in, mix_out, preferred_element_type=jnp.float32)
    out_mixer = row_norm(mixed, gain_mixer, bias_mixer)
    flat_ids = route_ids.reshape(-1).astype(jnp.int32)
    count_all = flat_ids.shape[0]
    order = jnp.argsort(flat_ids, stable=True).astype(jnp.int32)
    marks = (flat_ids[:, None] == jnp.arange(EXPERTS, dtype=jnp.int32)[None, :]).astype(jnp.int32)
    counts = lax.optimization_barrier(jnp.sum(marks, axis=0)).astype(jnp.int32)
    starts = (jnp.cumsum(counts) - counts).astype(jnp.int32)
    most_rows = N_EP * CAP

    def one_expert(results, expert):
        slots = jnp.arange(most_rows, dtype=jnp.int32)
        picks = jnp.clip(starts[expert] + slots, 0, count_all - 1).astype(jnp.int32)
        assigned = order[picks]
        valid = slots < counts[expert]
        inputs = moe_input[assigned // TOPK]
        gate_value = jnp.dot(inputs, expert_gate[expert], preferred_element_type=jnp.float32)
        up_value = jnp.dot(inputs, expert_up[expert], preferred_element_type=jnp.float32)
        hidden = (jax.nn.silu(gate_value) * up_value).astype(jnp.bfloat16)
        output = jnp.dot(hidden, expert_down[expert], preferred_element_type=jnp.float32).astype(jnp.bfloat16)
        target = jnp.where(valid, assigned, count_all).astype(jnp.int32)
        return (results.at[target].set(output, mode='drop'), None)
    empty = jnp.zeros((count_all, D), jnp.bfloat16)
    routed = lax.scan(one_expert, empty, jnp.arange(EXPERTS, dtype=jnp.int32))[0]
    shared_gate_value = jnp.dot(moe_input, shared_gate, preferred_element_type=jnp.float32)
    shared_up_value = jnp.dot(moe_input, shared_up, preferred_element_type=jnp.float32)
    shared_hidden = (jax.nn.silu(shared_gate_value) * shared_up_value).astype(jnp.bfloat16)
    shared_sum = jnp.dot(shared_hidden, shared_down, preferred_element_type=jnp.float32)
    weighted = routed.reshape(-1, TOPK, D).astype(jnp.float32) * route_weights.astype(jnp.float32)[:, :, None]
    combined = lax.optimization_barrier(jnp.sum(weighted, axis=1)) + shared_sum
    out_experts = row_norm(combined, gain_experts, bias_experts)
    return (out_mixer, out_experts)
```

```python
import functools

import jax
import jax.numpy as jnp
from jax import lax
from jax.experimental import pallas as pl
from jax.experimental.pallas import tpu as pltpu
from jax.sharding import PartitionSpec as P

SEQS = 1


def shifted(block, axis, distance):
    devices = range(lax.axis_size(axis))
    route = [(i - distance, i) for i in devices if i - distance in devices]
    return lax.ppermute(block, axis, route)


def finish(values, totals, squares, full_width, gain, offset_bias):
    average = (totals / full_width)[:, None]
    spread = (squares / full_width)[:, None] - average * average
    scaled = (values - average) * lax.rsqrt(spread + 1e-05)
    return (scaled * gain.astype(jnp.float32) + offset_bias.astype(jnp.float32)).astype(
        jnp.bfloat16
    )


def plain_device(
    outer_gate,
    inner_gate,
    conv_value,
    conv_taps,
    mix_out,
    gain_mixer,
    bias_mixer,
    moe_input,
    route_ids,
    route_weights,
    expert_gate,
    expert_up,
    expert_down,
    shared_gate,
    shared_up,
    shared_down,
    gain_experts,
    bias_experts,
):
    token_rows = outer_gate.shape[0]
    column_count = outer_gate.shape[1]
    ep_count = lax.axis_size("ep")
    tp_count = lax.axis_size("tp")
    taps_count = conv_taps.shape[0]
    product = (inner_gate.astype(jnp.float32) * conv_value.astype(jnp.float32)).astype(jnp.bfloat16)
    border = shifted(product[token_rows - (taps_count - 1) :], "ep", 1)
    extended = jnp.concatenate([border, product], axis=0).astype(jnp.float32)
    seq_length = token_rows * ep_count // SEQS
    places = (
        lax.axis_index("ep") * token_rows + jnp.arange(token_rows, dtype=jnp.int32)
    ) % seq_length
    convolved = jnp.zeros((token_rows, column_count), jnp.float32)
    for offset in range(taps_count):
        delay_rows = taps_count - 1 - offset
        delayed = extended[offset : offset + token_rows]
        kept_mask = (places >= delay_rows).astype(jnp.float32)[:, None]
        convolved = convolved + conv_taps[offset].astype(jnp.float32)[None, :] * delayed * kept_mask
    weighted_in = (outer_gate.astype(jnp.float32) * convolved).astype(jnp.bfloat16)
    block = mix_out
    mixed = jnp.dot(
        lax.all_gather(weighted_in, "tp", axis=1, tiled=True),
        block,
        preferred_element_type=jnp.float32,
    )
    topk_count = route_ids.shape[1]
    local_experts = expert_gate.shape[0]
    expert_count = local_experts * ep_count
    capacity = max(2, 3 * token_rows * topk_count // (2 * expert_count))
    flat_ids = route_ids.reshape(-1)
    marks = (flat_ids[:, None] == jnp.arange(expert_count, dtype=jnp.int32)[None, :]).astype(
        jnp.int32
    )
    ranks = jnp.sum((jnp.cumsum(marks, axis=0) - marks) * marks, axis=1)
    targets = flat_ids * capacity + ranks
    sources = jnp.arange(flat_ids.shape[0], dtype=jnp.int32) // topk_count
    sent_rows = lax.dynamic_slice_in_dim(
        moe_input, lax.axis_index("tp") * column_count, column_count, 1
    )
    buffer_rows = jnp.zeros((expert_count * capacity, sent_rows.shape[1]), jnp.bfloat16)
    buffer_rows = buffer_rows.at[targets].set(sent_rows[sources])
    sectioned = buffer_rows.reshape(ep_count, local_experts * capacity, sent_rows.shape[1])
    arrived = lax.all_to_all(sectioned, "ep", split_axis=0, concat_axis=0, tiled=True)
    arrived = lax.all_gather(arrived, "tp", axis=2, tiled=True)
    expert_rows = arrived.reshape(ep_count, local_experts, capacity, arrived.shape[2])
    gate_value = jnp.einsum(
        "secd,edf->secf", expert_rows, expert_gate, preferred_element_type=jnp.float32
    )
    up_value = jnp.einsum(
        "secd,edf->secf", expert_rows, expert_up, preferred_element_type=jnp.float32
    )
    hidden = (jax.nn.silu(gate_value) * up_value).astype(jnp.bfloat16)
    flat_hidden = hidden.reshape(expert_count * capacity, hidden.shape[3])
    shared_gate_value = jnp.dot(moe_input, shared_gate, preferred_element_type=jnp.float32)
    shared_up_value = jnp.dot(moe_input, shared_up, preferred_element_type=jnp.float32)
    shared_hidden = (jax.nn.silu(shared_gate_value) * shared_up_value).astype(jnp.bfloat16)
    piece = lax.all_gather(flat_hidden, "tp", axis=1, tiled=True)
    block = expert_down
    shaped = piece.reshape(ep_count, local_experts, capacity, piece.shape[1])
    routed_sum = jnp.einsum("secf,efd->secd", shaped, block, preferred_element_type=jnp.float32)
    block = shared_down
    shared_sum = jnp.dot(
        lax.all_gather(shared_hidden, "tp", axis=1, tiled=True),
        block,
        preferred_element_type=jnp.float32,
    )
    expert_out = routed_sum.astype(jnp.bfloat16).reshape(
        ep_count, local_experts * capacity, column_count
    )
    returned = lax.all_to_all(expert_out, "ep", split_axis=0, concat_axis=0, tiled=True)
    picked = returned.reshape(expert_count * capacity, column_count)[targets].astype(jnp.float32)
    weighted = picked.reshape(token_rows, topk_count, column_count) * route_weights[:, :, None]
    combined = jnp.sum(weighted, axis=1) + shared_sum
    mixer_total, mixer_square, expert_total, expert_square = lax.psum(
        (
            jnp.sum(mixed, axis=1),
            jnp.sum(mixed * mixed, axis=1),
            jnp.sum(combined, axis=1),
            jnp.sum(combined * combined, axis=1),
        ),
        "tp",
    )
    full_width = column_count * tp_count
    out_mixer = finish(mixed, mixer_total, mixer_square, full_width, gain_mixer, bias_mixer)
    out_experts = finish(
        combined, expert_total, expert_square, full_width, gain_experts, bias_experts
    )
    return (out_mixer, out_experts)


PLANE = 2
CORES = 2
VMEM_BYTES = 60 * 1024 * 1024


def silu(value):
    return value / (1.0 + jnp.exp(-value))


def fused_kernel(
    shape,
    outer_ref,
    inner_ref,
    value_ref,
    taps_ref,
    mix_hbm,
    gain_m_ref,
    bias_m_ref,
    moe_ref,
    weights_ref,
    gate_hbm,
    up_hbm,
    down_hbm,
    shared_gate_hbm,
    shared_up_hbm,
    shared_down_hbm,
    gain_e_ref,
    bias_e_ref,
    out_m_ref,
    out_e_ref,
    mix_v,
    gate_v,
    up_v,
    down_v,
    shared_gate_v,
    shared_up_v,
    shared_down_v,
    tokens,
    route,
    rows_in,
    hidden,
    weighted,
    shared_hidden,
    border,
    edge,
    extended,
    peer_part,
    own_part,
    sent_sum,
    returned,
    stats_out,
    stats_in,
    mixed_ref,
    total_ref,
    load_sem,
    send_sem,
    recv_sem,
):
    ep_count, tp_count, capacity, seq_length = shape
    chips = ep_count // CORES
    rows, cols = outer_ref.shape
    full_width = cols * tp_count
    me = lax.axis_index("ep")
    j = lax.axis_index("tp")
    z = me // CORES
    c = me % CORES
    x = j % PLANE
    y = j // PLANE
    jx = y * PLANE + (1 - x)
    jy = (1 - y) * PLANE + x
    jd = (1 - y) * PLANE + (1 - x)
    other = z * CORES + (1 - c)
    f32, bf16 = jnp.float32, jnp.bfloat16

    order = (
        (shared_gate_hbm, shared_gate_v),
        (shared_up_hbm, shared_up_v),
        (gate_hbm.at[0], gate_v),
        (up_hbm.at[0], up_v),
        (mix_hbm, mix_v),
        (down_hbm.at[0], down_v),
        (shared_down_hbm, shared_down_v),
    )
    loads = [pltpu.make_async_copy(a, b, load_sem.at[n]) for n, (a, b) in enumerate(order)]
    for load in loads:
        load.start()

    product = (inner_ref[...].astype(f32) * value_ref[...].astype(f32)).astype(bf16)
    edge_rows = edge.shape[0]
    edge[...] = product[rows - edge_rows :]
    pad = extended.shape[0] - rows
    extended[pad:, :] = product.astype(f32)
    route[0, 0] = weights_ref[...]

    barrier = pltpu.get_barrier_semaphore()
    for step in range(1, ep_count):
        pl.semaphore_signal(barrier, inc=1, device_id=((me + step) % ep_count, j), device_id_type=pl.DeviceIdType.MESH)
    for peer in (jx, jy, jd):
        pl.semaphore_signal(barrier, inc=1, device_id=(me, peer), device_id_type=pl.DeviceIdType.MESH)
    pl.semaphore_wait(barrier, ep_count - 1 + tp_count - 1)

    numbers = {}
    started = []

    def number(name):
        return numbers.setdefault(name, len(numbers))

    def copy(name, source, target, device):
        n = number(name)
        return pltpu.make_async_remote_copy(
            src_ref=source,
            dst_ref=target,
            send_sem=send_sem.at[n],
            recv_sem=recv_sem.at[n],
            device_id=device,
            device_id_type=pl.DeviceIdType.MESH,
        )

    def send(name, source, target, device):
        c_ = copy(name, source, target, device)
        c_.start()
        started.append(c_)

    def arrive(name, target):
        copy(name, target, target, (other, j)).wait_recv()

    def columns(owner):
        return pl.ds(pl.multiple_of(owner * cols, cols), cols)

    def gather_start(name, ref):
        part = ref.at[:, columns(j)]
        send(name + ("x",), part, part, (me, jx))
        send(name + ("y",), part, part, (me, jy))

    def gather_relay(name, ref):
        half = ref.shape[0] // 2
        arrive(name + ("x",), ref.at[:, columns(jx)])
        part = ref.at[pl.ds(0, half), columns(jx)]
        send(name + ("xy",), part, part, (me, jy))
        arrive(name + ("y",), ref.at[:, columns(jy)])
        part = ref.at[pl.ds(half, half), columns(jy)]
        send(name + ("yx",), part, part, (me, jx))

    def gather_finish(name, ref):
        half = ref.shape[0] // 2
        arrive(name + ("xy",), ref.at[pl.ds(0, half), columns(jd)])
        arrive(name + ("yx",), ref.at[pl.ds(half, half), columns(jd)])

    send(("pair", 0), moe_ref, tokens.at[0, 1], (other, j))
    for s in range(chips):
        target = (z - s + chips) % chips
        if s > 0:
            send(("route", s, 0), weights_ref, route.at[s, 0], (target * CORES + c, j))
        send(("route", s, 1), weights_ref, route.at[s, 1], (target * CORES + (1 - c), j))
    for s in range(1, chips):
        target = (z - s + chips) % chips
        send(
            ("line", s),
            moe_ref.at[:, columns(j)],
            tokens.at[s, 0, :, columns(j)],
            (target * CORES + c, j),
        )
    send(("edge",), edge, border, ((me + 1) % ep_count, j))

    def dot(a, b):
        return jnp.dot(a, b, preferred_element_type=f32)

    loads[0].wait()
    loads[1].wait()
    held = silu(dot(moe_ref[...], shared_gate_v[...])) * dot(moe_ref[...], shared_up_v[...])
    shared_hidden[:, columns(j)] = held.astype(bf16)
    gather_start(("shared",), shared_hidden)

    arrive(("edge",), border)
    extended[pad - edge_rows : pad, :] = border[...].astype(f32)
    places = (me * rows + lax.broadcasted_iota(jnp.int32, (rows, 1), 0)) % seq_length
    taps_count = taps_ref.shape[0]
    convolved = jnp.zeros((rows, cols), f32)
    for offset in range(taps_count):
        delay = taps_count - 1 - offset
        delayed = extended[pad - delay : pad - delay + rows, :]
        kept = (places >= delay).astype(f32)
        convolved = convolved + taps_ref[offset : offset + 1, :].astype(f32) * delayed * kept
    weighted[:, columns(j)] = (outer_ref[...].astype(f32) * convolved).astype(bf16)
    gather_start(("mixer",), weighted)

    def token_ref(s, p):
        return moe_ref if (s, p) == (0, 0) else tokens.at[s, p]

    def choice(s, p):
        weight = route[s, p, pl.ds(me, 1), :]
        routed = (weight > 0.0).astype(f32)
        earlier = lax.broadcasted_iota(jnp.int32, (rows, rows), 0)
        later = lax.broadcasted_iota(jnp.int32, (rows, rows), 1)
        upper = (earlier <= later).astype(f32).astype(bf16)
        many = jnp.broadcast_to(routed, (16, rows)).astype(bf16)
        rank = dot(many, upper)[0:1, :] * routed
        slot = lax.broadcasted_iota(jnp.int32, (capacity, rows), 0).astype(f32) + 1.0
        return (slot == rank).astype(f32), weight

    def expert_up_stage(s):
        for p in range(CORES):
            picks, _ = choice(s, p)
            rows_in[p * capacity : (p + 1) * capacity, :] = dot(
                picks.astype(bf16), token_ref(s, p)[...]
            ).astype(bf16)
        held = silu(dot(rows_in[...], gate_v[...])) * dot(rows_in[...], up_v[...])
        hidden[s, :, columns(j)] = held.astype(bf16)
        gather_start(("hidden", s), hidden.at[s])

    def expert_down_stage(s):
        full = dot(hidden[s], down_v[...])
        for p in reversed(range(CORES)):
            picks, weight = choice(s, p)
            scale = jnp.sum(picks * weight, axis=1, keepdims=True)
            scaled = (full[p * capacity : (p + 1) * capacity] * scale).astype(bf16)
            spread = lax.dot_general(
                picks.astype(bf16), scaled, (((0,), (0,)), ((), ())), preferred_element_type=f32
            )
            if p == 1:
                own_part[s] = spread.astype(bf16)
                send(("part", s), own_part.at[s], peer_part.at[s], (other, j))
            elif s == 0:
                total_ref[...] = spread
            else:
                sent_sum[s] = spread.astype(bf16)

    def expert_return(s):
        arrive(("part", s), peer_part.at[s])
        if s == 0:
            total_ref[...] = total_ref[...] + peer_part[0].astype(f32)
        else:
            sent_sum[s] = (sent_sum[s].astype(f32) + peer_part[s].astype(f32)).astype(bf16)
            target = (z + s) % chips
            send(("return", s), sent_sum.at[s], returned.at[s], (target * CORES + c, j))

    def wait_routes(s):
        for p in range(CORES):
            if (s, p) != (0, 0):
                arrive(("route", s, p), route.at[s, p])

    def pair_tokens(s):
        gather_finish(("tokens", s), tokens.at[s, 0])
        send(("pair", s), tokens.at[s, 0], tokens.at[s, 1], (other, j))

    def line_tokens(s):
        arrive(("line", s), tokens.at[s, 0, :, columns(j)])
        gather_start(("tokens", s), tokens.at[s, 0])

    def stats_start(k, values):
        lane = lax.broadcasted_iota(jnp.int32, (rows, rows), 1)
        total = jnp.sum(values, axis=1, keepdims=True)
        square = jnp.sum(values * values, axis=1, keepdims=True)
        tile = jnp.where(lane == 0, total, jnp.where(lane == 1, square, 0.0))
        stats_out[k] = tile.T[0 : stats_out.shape[1], :]
        for n, peer in enumerate((jx, jy, jd)):
            send(("stats", k, n), stats_out.at[k], stats_in.at[k, n], (me, peer))

    def stats_finish(k, values, gain_ref, bias_ref, out_ref):
        tile = stats_out[k]
        for n in range(tp_count - 1):
            arrive(("stats", k, n), stats_in.at[k, n])
            tile = tile + stats_in[k, n]
        padded = jnp.concatenate(
            [tile, jnp.zeros((rows - tile.shape[0], rows), f32)], axis=0
        ).T
        average = padded[:, 0:1] / full_width
        spread = padded[:, 1:2] / full_width - average * average
        scaled = (values - average) * lax.rsqrt(spread + 1e-05)
        out_ref[...] = (
            scaled * gain_ref[...].astype(f32) + bias_ref[...].astype(f32)
        ).astype(bf16)

    wait_routes(0)
    arrive(("pair", 0), tokens.at[0, 1])
    loads[2].wait()
    loads[3].wait()
    expert_up_stage(0)
    for s in range(1, chips):
        line_tokens(s)
        if s == 1:
            gather_relay(("shared",), shared_hidden)
            gather_relay(("mixer",), weighted)
    gather_relay(("tokens", 1), tokens.at[1, 0])
    gather_relay(("hidden", 0), hidden.at[0])
    for s in range(1, chips):
        pair_tokens(s)
        if s == 1:
            gather_finish(("mixer",), weighted)
            loads[4].wait()
            mixed_ref[...] = dot(weighted[...], mix_v[...])
            stats_start(0, mixed_ref[...])
        if s + 1 < chips:
            gather_relay(("tokens", s + 1), tokens.at[s + 1, 0])
        wait_routes(s)
        arrive(("pair", s), tokens.at[s, 1])
        expert_up_stage(s)
        if s == 1:
            loads[5].wait()
        gather_finish(("hidden", s - 1), hidden.at[s - 1])
        expert_down_stage(s - 1)
        gather_relay(("hidden", s), hidden.at[s])
        expert_return(s - 1)
    gather_finish(("shared",), shared_hidden)
    loads[6].wait()
    total_ref[...] = total_ref[...] + dot(shared_hidden[...], shared_down_v[...])
    stats_finish(0, mixed_ref[...], gain_m_ref, bias_m_ref, out_m_ref)
    last = chips - 1
    gather_finish(("hidden", last), hidden.at[last])
    expert_down_stage(last)
    expert_return(last)
    combined = total_ref[...]
    for s in range(1, chips):
        arrive(("return", s), returned.at[s])
        combined = combined + returned[s].astype(f32)
    stats_start(1, combined)
    total_ref[...] = combined
    stats_finish(1, total_ref[...], gain_e_ref, bias_e_ref, out_e_ref)
    for item in started:
        item.wait_send()


def fused_device(
    outer_gate,
    inner_gate,
    conv_value,
    conv_taps,
    mix_out,
    gain_mixer,
    bias_mixer,
    moe_input,
    route_ids,
    route_weights,
    expert_gate,
    expert_up,
    expert_down,
    shared_gate,
    shared_up,
    shared_down,
    gain_experts,
    bias_experts,
):
    rows, cols = outer_gate.shape
    width = moe_input.shape[1]
    ep_count = lax.axis_size("ep")
    tp_count = lax.axis_size("tp")
    chips = ep_count // CORES
    capacity = max(2, 3 * rows * route_ids.shape[1] // (2 * ep_count))
    seq_length = rows * ep_count // SEQS
    experts = jnp.arange(ep_count, dtype=jnp.int32)
    named = route_ids.T[None, :, :] == experts[:, None, None]
    dense = jnp.sum(jnp.where(named, route_weights.T[None, :, :], 0.0), axis=1)
    bf16, f32 = jnp.bfloat16, jnp.float32
    vmem = pl.BlockSpec(memory_space=pltpu.VMEM)
    hbm = pl.BlockSpec(memory_space=pl.ANY)
    copies = 16 * chips + 24
    weight = pltpu.VMEM((width, cols), bf16)
    scratch = [
        *([weight] * 7),
        pltpu.VMEM((chips, CORES, rows, width), bf16),
        pltpu.VMEM((chips, CORES, ep_count, rows), f32),
        pltpu.VMEM((CORES * capacity, width), bf16),
        pltpu.VMEM((chips, CORES * capacity, width), bf16),
        pltpu.VMEM((rows, width), bf16),
        pltpu.VMEM((rows, width), bf16),
        pltpu.VMEM((16, cols), bf16),
        pltpu.VMEM((16, cols), bf16),
        pltpu.VMEM((rows + 16, cols), f32),
        pltpu.VMEM((chips, rows, cols), bf16),
        pltpu.VMEM((chips, rows, cols), bf16),
        pltpu.VMEM((chips, rows, cols), bf16),
        pltpu.VMEM((chips, rows, cols), bf16),
        pltpu.VMEM((2, 8, rows), f32),
        pltpu.VMEM((2, tp_count - 1, 8, rows), f32),
        pltpu.VMEM((rows, cols), f32),
        pltpu.VMEM((rows, cols), f32),
        pltpu.SemaphoreType.DMA((7,)),
        pltpu.SemaphoreType.DMA((copies,)),
        pltpu.SemaphoreType.DMA((copies,)),
    ]
    out = jax.ShapeDtypeStruct((rows, cols), bf16)
    return pl.pallas_call(
        functools.partial(fused_kernel, (ep_count, tp_count, capacity, seq_length)),
        out_shape=(out, out),
        in_specs=[vmem, vmem, vmem, vmem, hbm, vmem, vmem, vmem, vmem]
        + [hbm] * 6
        + [vmem, vmem],
        out_specs=(vmem, vmem),
        scratch_shapes=scratch,
        compiler_params=pltpu.CompilerParams(
            collective_id=0, has_side_effects=True, vmem_limit_bytes=VMEM_BYTES
        ),
    )(
        outer_gate,
        inner_gate,
        conv_value,
        conv_taps,
        mix_out,
        gain_mixer.reshape(1, cols),
        bias_mixer.reshape(1, cols),
        moe_input,
        dense,
        expert_gate,
        expert_up,
        expert_down,
        shared_gate,
        shared_up,
        shared_down,
        gain_experts.reshape(1, cols),
        bias_experts.reshape(1, cols),
    )


def on_device(*arrays):
    local_experts = arrays[10].shape[0]
    square = lax.axis_size("tp") == PLANE * PLANE
    if square and local_experts == 1 and lax.axis_size("ep") % CORES == 0:
        return fused_device(*arrays)
    return plain_device(*arrays)


def solution(mesh):
    in_specs = (
        P("ep", "tp"),
        P("ep", "tp"),
        P("ep", "tp"),
        P(None, "tp"),
        P(None, "tp"),
        P("tp"),
        P("tp"),
        P("ep", None),
        P("ep", None),
        P("ep", None),
        P("ep", None, "tp"),
        P("ep", None, "tp"),
        P("ep", None, "tp"),
        P(None, "tp"),
        P(None, "tp"),
        P(None, "tp"),
        P("tp"),
        P("tp"),
    )
    out_specs = (P("ep", "tp"), P("ep", "tp"))
    return jax.shard_map(
        on_device, mesh=mesh, in_specs=in_specs, out_specs=out_specs, check_vma=False
    )
```

```python
import functools

import jax
import jax.numpy as jnp
from jax import lax
from jax.experimental import pallas as pl
from jax.experimental.pallas import tpu as pltpu
from jax.sharding import PartitionSpec as P

SEQS = 1


def shifted(block, axis, distance):
    devices = range(lax.axis_size(axis))
    route = [(i - distance, i) for i in devices if i - distance in devices]
    return lax.ppermute(block, axis, route)


def finish(values, totals, squares, full_width, gain, offset_bias):
    average = (totals / full_width)[:, None]
    spread = (squares / full_width)[:, None] - average * average
    scaled = (values - average) * lax.rsqrt(spread + 1e-05)
    return (scaled * gain.astype(jnp.float32) + offset_bias.astype(jnp.float32)).astype(
        jnp.bfloat16
    )


def plain_device(
    outer_gate,
    inner_gate,
    conv_value,
    conv_taps,
    mix_out,
    gain_mixer,
    bias_mixer,
    moe_input,
    route_ids,
    route_weights,
    expert_gate,
    expert_up,
    expert_down,
    shared_gate,
    shared_up,
    shared_down,
    gain_experts,
    bias_experts,
):
    token_rows = outer_gate.shape[0]
    column_count = outer_gate.shape[1]
    ep_count = lax.axis_size("ep")
    tp_count = lax.axis_size("tp")
    taps_count = conv_taps.shape[0]
    product = (inner_gate.astype(jnp.float32) * conv_value.astype(jnp.float32)).astype(jnp.bfloat16)
    border = shifted(product[token_rows - (taps_count - 1) :], "ep", 1)
    extended = jnp.concatenate([border, product], axis=0).astype(jnp.float32)
    seq_length = token_rows * ep_count // SEQS
    places = (
        lax.axis_index("ep") * token_rows + jnp.arange(token_rows, dtype=jnp.int32)
    ) % seq_length
    convolved = jnp.zeros((token_rows, column_count), jnp.float32)
    for offset in range(taps_count):
        delay_rows = taps_count - 1 - offset
        delayed = extended[offset : offset + token_rows]
        kept_mask = (places >= delay_rows).astype(jnp.float32)[:, None]
        convolved = convolved + conv_taps[offset].astype(jnp.float32)[None, :] * delayed * kept_mask
    weighted_in = (outer_gate.astype(jnp.float32) * convolved).astype(jnp.bfloat16)
    block = mix_out
    mixed = jnp.dot(
        lax.all_gather(weighted_in, "tp", axis=1, tiled=True),
        block,
        preferred_element_type=jnp.float32,
    )
    topk_count = route_ids.shape[1]
    local_experts = expert_gate.shape[0]
    expert_count = local_experts * ep_count
    capacity = max(2, 3 * token_rows * topk_count // (2 * expert_count))
    flat_ids = route_ids.reshape(-1)
    marks = (flat_ids[:, None] == jnp.arange(expert_count, dtype=jnp.int32)[None, :]).astype(
        jnp.int32
    )
    ranks = jnp.sum((jnp.cumsum(marks, axis=0) - marks) * marks, axis=1)
    targets = flat_ids * capacity + ranks
    sources = jnp.arange(flat_ids.shape[0], dtype=jnp.int32) // topk_count
    sent_rows = lax.dynamic_slice_in_dim(
        moe_input, lax.axis_index("tp") * column_count, column_count, 1
    )
    buffer_rows = jnp.zeros((expert_count * capacity, sent_rows.shape[1]), jnp.bfloat16)
    buffer_rows = buffer_rows.at[targets].set(sent_rows[sources])
    sectioned = buffer_rows.reshape(ep_count, local_experts * capacity, sent_rows.shape[1])
    arrived = lax.all_to_all(sectioned, "ep", split_axis=0, concat_axis=0, tiled=True)
    arrived = lax.all_gather(arrived, "tp", axis=2, tiled=True)
    expert_rows = arrived.reshape(ep_count, local_experts, capacity, arrived.shape[2])
    gate_value = jnp.einsum(
        "secd,edf->secf", expert_rows, expert_gate, preferred_element_type=jnp.float32
    )
    up_value = jnp.einsum(
        "secd,edf->secf", expert_rows, expert_up, preferred_element_type=jnp.float32
    )
    hidden = (jax.nn.silu(gate_value) * up_value).astype(jnp.bfloat16)
    flat_hidden = hidden.reshape(expert_count * capacity, hidden.shape[3])
    shared_gate_value = jnp.dot(moe_input, shared_gate, preferred_element_type=jnp.float32)
    shared_up_value = jnp.dot(moe_input, shared_up, preferred_element_type=jnp.float32)
    shared_hidden = (jax.nn.silu(shared_gate_value) * shared_up_value).astype(jnp.bfloat16)
    piece = lax.all_gather(flat_hidden, "tp", axis=1, tiled=True)
    block = expert_down
    shaped = piece.reshape(ep_count, local_experts, capacity, piece.shape[1])
    routed_sum = jnp.einsum("secf,efd->secd", shaped, block, preferred_element_type=jnp.float32)
    block = shared_down
    shared_sum = jnp.dot(
        lax.all_gather(shared_hidden, "tp", axis=1, tiled=True),
        block,
        preferred_element_type=jnp.float32,
    )
    expert_out = routed_sum.astype(jnp.bfloat16).reshape(
        ep_count, local_experts * capacity, column_count
    )
    returned = lax.all_to_all(expert_out, "ep", split_axis=0, concat_axis=0, tiled=True)
    picked = returned.reshape(expert_count * capacity, column_count)[targets].astype(jnp.float32)
    weighted = picked.reshape(token_rows, topk_count, column_count) * route_weights[:, :, None]
    combined = jnp.sum(weighted, axis=1) + shared_sum
    mixer_total, mixer_square, expert_total, expert_square = lax.psum(
        (
            jnp.sum(mixed, axis=1),
            jnp.sum(mixed * mixed, axis=1),
            jnp.sum(combined, axis=1),
            jnp.sum(combined * combined, axis=1),
        ),
        "tp",
    )
    full_width = column_count * tp_count
    out_mixer = finish(mixed, mixer_total, mixer_square, full_width, gain_mixer, bias_mixer)
    out_experts = finish(
        combined, expert_total, expert_square, full_width, gain_experts, bias_experts
    )
    return (out_mixer, out_experts)


PLANE = 2
CORES = 2
VMEM_BYTES = 60 * 1024 * 1024


def plan(chips):
    steps = [("shared", 0), ("up", 0), ("hidden", 0)]
    waiting = [("shared_relay", 0), ("mixer", 0)]
    for s in range(1, chips):
        steps.append(("line", s))
        steps += waiting
        waiting = [("token_relay", 1), ("hidden_relay", 0)] if s == 1 else []
    steps += waiting + [("pair", 1)]
    for s in range(1, chips):
        if s + 1 < chips:
            steps.append(("token_relay", s + 1))
        if s == 1:
            steps.append(("mixer_relay", 0))
        if s == 2:
            steps += [("mixer_dot", 0), ("hidden_relay", 1)]
        if s > 1:
            steps.append(("pair", s))
        steps += [("up", s), ("hidden", s)]
        if s > 2:
            steps.append(("hidden_relay", s - 1))
    steps.append(("shared_dot", 0))
    for s in range(chips):
        steps.append(("down", s))
        if s == 0:
            steps.append(("hidden_relay", chips - 1))
        if s == chips - 2:
            steps.append(("mixer_end", 0))
        steps.append(("return", s))
    return steps + [("collect", s) for s in range(1, chips)]


def silu(value):
    return value / (1.0 + jnp.exp(-value))


def fused_kernel(
    shape,
    outer_ref,
    inner_ref,
    value_ref,
    taps_ref,
    mix_hbm,
    gain_m_ref,
    bias_m_ref,
    moe_ref,
    ids_ref,
    route_w_ref,
    gate_hbm,
    up_hbm,
    down_hbm,
    shared_gate_hbm,
    shared_up_hbm,
    shared_down_hbm,
    gain_e_ref,
    bias_e_ref,
    out_m_ref,
    out_e_ref,
    mix_v,
    gate_v,
    up_v,
    down_v,
    shared_gate_v,
    shared_up_v,
    shared_down_v,
    tokens,
    route,
    rows_in,
    hidden,
    weighted,
    shared_hidden,
    border,
    edge,
    extended,
    peer_part,
    own_part,
    sent_sum,
    returned,
    stats_out,
    stats_in,
    mixed_ref,
    total_ref,
    load_sem,
    send_sem,
    recv_sem,
):
    ep_count, tp_count, capacity, seq_length = shape
    chips = ep_count // CORES
    rows, cols = outer_ref.shape
    full_width = cols * tp_count
    me = lax.axis_index("ep")
    j = lax.axis_index("tp")
    z = me // CORES
    c = me % CORES
    x = j % PLANE
    y = j // PLANE
    jx = y * PLANE + (1 - x)
    jy = (1 - y) * PLANE + x
    jd = (1 - y) * PLANE + (1 - x)
    other = z * CORES + (1 - c)
    f32, bf16 = jnp.float32, jnp.bfloat16

    order = (
        (shared_gate_hbm, shared_gate_v),
        (shared_up_hbm, shared_up_v),
        (gate_hbm.at[0], gate_v),
        (up_hbm.at[0], up_v),
        (mix_hbm, mix_v),
        (down_hbm.at[0], down_v),
        (shared_down_hbm, shared_down_v),
    )
    loads = [pltpu.make_async_copy(a, b, load_sem.at[n]) for n, (a, b) in enumerate(order)]
    for load in loads:
        load.start()

    product = (inner_ref[...].astype(f32) * value_ref[...].astype(f32)).astype(bf16)
    edge_rows = edge.shape[0]
    edge[...] = product[rows - edge_rows :]
    pad = extended.shape[0] - rows
    extended[pad:, :] = product.astype(f32)
    named = lax.broadcasted_iota(jnp.int32, (ep_count, rows), 0)
    dense = jnp.zeros((ep_count, rows), f32)
    for k in range(ids_ref.shape[0]):
        dense = dense + jnp.where(named == ids_ref[k : k + 1, :], route_w_ref[k : k + 1, :], 0.0)
    route[0, 0] = dense

    barrier = pltpu.get_barrier_semaphore()
    for step in range(1, ep_count):
        pl.semaphore_signal(barrier, inc=1, device_id=((me + step) % ep_count, j), device_id_type=pl.DeviceIdType.MESH)
    for peer in (jx, jy, jd):
        pl.semaphore_signal(barrier, inc=1, device_id=(me, peer), device_id_type=pl.DeviceIdType.MESH)
    pl.semaphore_wait(barrier, ep_count - 1 + tp_count - 1)

    numbers = {}
    started = []

    def number(name):
        return numbers.setdefault(name, len(numbers))

    def copy(name, source, target, device):
        n = number(name)
        return pltpu.make_async_remote_copy(
            src_ref=source,
            dst_ref=target,
            send_sem=send_sem.at[n],
            recv_sem=recv_sem.at[n],
            device_id=device,
            device_id_type=pl.DeviceIdType.MESH,
        )

    def send(name, source, target, device):
        c_ = copy(name, source, target, device)
        c_.start()
        started.append(c_)

    def arrive(name, target):
        copy(name, target, target, (other, j)).wait_recv()

    def columns(owner):
        return pl.ds(pl.multiple_of(owner * cols, cols), cols)

    def gather_start(name, ref):
        part = ref.at[:, columns(j)]
        send(name + ("x",), part, part, (me, jx))
        send(name + ("y",), part, part, (me, jy))

    def gather_relay(name, ref):
        half = ref.shape[0] // 2
        arrive(name + ("x",), ref.at[:, columns(jx)])
        part = ref.at[pl.ds(0, half), columns(jx)]
        send(name + ("xy",), part, part, (me, jy))
        arrive(name + ("y",), ref.at[:, columns(jy)])
        part = ref.at[pl.ds(half, half), columns(jy)]
        send(name + ("yx",), part, part, (me, jx))

    def gather_finish(name, ref):
        half = ref.shape[0] // 2
        arrive(name + ("xy",), ref.at[pl.ds(0, half), columns(jd)])
        arrive(name + ("yx",), ref.at[pl.ds(half, half), columns(jd)])

    send(("pair", 0), moe_ref, tokens.at[0, 1], (other, j))
    for s in range(chips):
        target = (z - s + chips) % chips
        if s > 0:
            send(("route", s, 0), route.at[0, 0], route.at[s, 0], (target * CORES + c, j))
        send(("route", s, 1), route.at[0, 0], route.at[s, 1], (target * CORES + (1 - c), j))
    for s in range(1, chips):
        target = (z - s + chips) % chips
        send(
            ("line", s),
            moe_ref.at[:, columns(j)],
            tokens.at[s, 0, :, columns(j)],
            (target * CORES + c, j),
        )
    send(("edge",), edge, border, ((me + 1) % ep_count, j))

    def dot(a, b):
        return jnp.dot(a, b, preferred_element_type=f32)

    def token_ref(s, p):
        return moe_ref if (s, p) == (0, 0) else tokens.at[s, p]

    def choice(s, p):
        weight = route[s, p, pl.ds(me, 1), :]
        routed = (weight > 0.0).astype(f32)
        earlier = lax.broadcasted_iota(jnp.int32, (rows, rows), 0)
        later = lax.broadcasted_iota(jnp.int32, (rows, rows), 1)
        upper = (earlier <= later).astype(f32).astype(bf16)
        many = jnp.broadcast_to(routed, (16, rows)).astype(bf16)
        rank = dot(many, upper)[0:1, :] * routed
        slot = lax.broadcasted_iota(jnp.int32, (capacity, rows), 0).astype(f32) + 1.0
        return (slot == rank).astype(f32), weight

    def expert_up_stage(s):
        for p in range(CORES):
            picks, _ = choice(s, p)
            rows_in[p * capacity : (p + 1) * capacity, :] = dot(
                picks.astype(bf16), token_ref(s, p)[...]
            ).astype(bf16)
        held = silu(dot(rows_in[...], gate_v[...])) * dot(rows_in[...], up_v[...])
        hidden[s, :, columns(j)] = held.astype(bf16)

    def hidden_start(s):
        gather_start(("hidden", s), hidden.at[s])

    def hidden_relay(s):
        gather_relay(("hidden", s), hidden.at[s])

    def token_relay(s):
        gather_relay(("tokens", s), tokens.at[s, 0])

    def collect(s):
        arrive(("return", s), returned.at[s])
        total_ref[...] = total_ref[...] + returned[s].astype(f32)

    def expert_down_stage(s):
        full = dot(hidden[s], down_v[...])
        for p in reversed(range(CORES)):
            picks, weight = choice(s, p)
            scale = jnp.sum(picks * weight, axis=1, keepdims=True)
            scaled = (full[p * capacity : (p + 1) * capacity] * scale).astype(bf16)
            spread = lax.dot_general(
                picks.astype(bf16), scaled, (((0,), (0,)), ((), ())), preferred_element_type=f32
            )
            if p == 1:
                own_part[s] = spread.astype(bf16)
                send(("part", s), own_part.at[s], peer_part.at[s], (other, j))
            elif s == 0:
                total_ref[...] = total_ref[...] + spread
            else:
                sent_sum[s] = spread.astype(bf16)

    def expert_return(s):
        arrive(("part", s), peer_part.at[s])
        if s == 0:
            total_ref[...] = total_ref[...] + peer_part[0].astype(f32)
        else:
            sent_sum[s] = (sent_sum[s].astype(f32) + peer_part[s].astype(f32)).astype(bf16)
            target = (z + s) % chips
            send(("return", s), sent_sum.at[s], returned.at[s], (target * CORES + c, j))

    def wait_routes(s):
        for p in range(CORES):
            if (s, p) != (0, 0):
                arrive(("route", s, p), route.at[s, p])

    def pair_tokens(s):
        gather_finish(("tokens", s), tokens.at[s, 0])
        send(("pair", s), tokens.at[s, 0], tokens.at[s, 1], (other, j))

    def line_tokens(s):
        arrive(("line", s), tokens.at[s, 0, :, columns(j)])
        gather_start(("tokens", s), tokens.at[s, 0])

    def stats_start(k, values):
        lane = lax.broadcasted_iota(jnp.int32, (rows, rows), 1)
        total = jnp.sum(values, axis=1, keepdims=True)
        square = jnp.sum(values * values, axis=1, keepdims=True)
        tile = jnp.where(lane == 0, total, jnp.where(lane == 1, square, 0.0))
        stats_out[k] = tile.T[0 : stats_out.shape[1], :]
        for n, peer in enumerate((jx, jy, jd)):
            send(("stats", k, n), stats_out.at[k], stats_in.at[k, n], (me, peer))

    def stats_finish(k, values, gain_ref, bias_ref, out_ref):
        tile = stats_out[k]
        for n in range(tp_count - 1):
            arrive(("stats", k, n), stats_in.at[k, n])
            tile = tile + stats_in[k, n]
        padded = jnp.concatenate(
            [tile, jnp.zeros((rows - tile.shape[0], rows), f32)], axis=0
        ).T
        average = padded[:, 0:1] / full_width
        spread = padded[:, 1:2] / full_width - average * average
        scaled = (values - average) * lax.rsqrt(spread + 1e-05)
        out_ref[...] = (
            scaled * gain_ref[...].astype(f32).reshape(1, cols)
            + bias_ref[...].astype(f32).reshape(1, cols)
        ).astype(bf16)

    def shared_start(_):
        loads[0].wait()
        loads[1].wait()
        held = silu(dot(moe_ref[...], shared_gate_v[...])) * dot(moe_ref[...], shared_up_v[...])
        shared_hidden[:, columns(j)] = held.astype(bf16)
        gather_start(("shared",), shared_hidden)

    def mixer_start(_):
        arrive(("edge",), border)
        extended[pad - edge_rows : pad, :] = border[...].astype(f32)
        places = (me * rows + lax.broadcasted_iota(jnp.int32, (rows, 1), 0)) % seq_length
        taps_count = taps_ref.shape[0]
        convolved = jnp.zeros((rows, cols), f32)
        for offset in range(taps_count):
            delay = taps_count - 1 - offset
            delayed = extended[pad - delay : pad - delay + rows, :]
            kept = (places >= delay).astype(f32)
            convolved = convolved + taps_ref[offset : offset + 1, :].astype(f32) * delayed * kept
        weighted[:, columns(j)] = (outer_ref[...].astype(f32) * convolved).astype(bf16)
        gather_start(("mixer",), weighted)

    def expert_up_start(s):
        wait_routes(s)
        arrive(("pair", s), tokens.at[s, 1])
        if s == 0:
            loads[2].wait()
            loads[3].wait()
        expert_up_stage(s)

    def shared_relay(_):
        gather_relay(("shared",), shared_hidden)

    def mixer_relay(_):
        gather_relay(("mixer",), weighted)

    def mixer_dot(_):
        gather_finish(("mixer",), weighted)
        loads[4].wait()
        mixed_ref[...] = dot(weighted[...], mix_v[...])
        stats_start(0, mixed_ref[...])

    def mixer_end(_):
        stats_finish(0, mixed_ref[...], gain_m_ref, bias_m_ref, out_m_ref)

    def shared_dot(_):
        gather_finish(("shared",), shared_hidden)
        loads[6].wait()
        total_ref[...] = dot(shared_hidden[...], shared_down_v[...])
        loads[5].wait()

    def expert_down(s):
        gather_finish(("hidden", s), hidden.at[s])
        expert_down_stage(s)

    acts = {
        "shared": shared_start,
        "mixer": mixer_start,
        "shared_relay": shared_relay,
        "mixer_relay": mixer_relay,
        "mixer_dot": mixer_dot,
        "mixer_end": mixer_end,
        "shared_dot": shared_dot,
        "line": line_tokens,
        "token_relay": token_relay,
        "pair": pair_tokens,
        "up": expert_up_start,
        "hidden": hidden_start,
        "hidden_relay": hidden_relay,
        "down": expert_down,
        "return": expert_return,
        "collect": collect,
    }
    for act, s in plan(chips):
        acts[act](s)
    stats_start(1, total_ref[...])
    stats_finish(1, total_ref[...], gain_e_ref, bias_e_ref, out_e_ref)
    for item in started:
        item.wait_send()


def pass_kernel(first_ref, second_ref, out_first_ref, out_second_ref):
    out_first_ref[...] = first_ref[...]
    out_second_ref[...] = second_ref[...]


def fused_device(
    outer_gate,
    inner_gate,
    conv_value,
    conv_taps,
    mix_out,
    gain_mixer,
    bias_mixer,
    moe_input,
    route_ids,
    route_weights,
    expert_gate,
    expert_up,
    expert_down,
    shared_gate,
    shared_up,
    shared_down,
    gain_experts,
    bias_experts,
):
    rows, cols = outer_gate.shape
    width = moe_input.shape[1]
    ep_count = lax.axis_size("ep")
    tp_count = lax.axis_size("tp")
    chips = ep_count // CORES
    capacity = max(2, 3 * rows * route_ids.shape[1] // (2 * ep_count))
    seq_length = rows * ep_count // SEQS
    bf16, f32 = jnp.bfloat16, jnp.float32
    vmem = pl.BlockSpec(memory_space=pltpu.VMEM)
    hbm = pl.BlockSpec(memory_space=pl.ANY)
    copies = 16 * chips + 24
    weight = pltpu.VMEM((width, cols), bf16)
    scratch = [
        *([weight] * 7),
        pltpu.VMEM((chips, CORES, rows, width), bf16),
        pltpu.VMEM((chips, CORES, ep_count, rows), f32),
        pltpu.VMEM((CORES * capacity, width), bf16),
        pltpu.VMEM((chips, CORES * capacity, width), bf16),
        pltpu.VMEM((rows, width), bf16),
        pltpu.VMEM((rows, width), bf16),
        pltpu.VMEM((16, cols), bf16),
        pltpu.VMEM((16, cols), bf16),
        pltpu.VMEM((rows + 16, cols), f32),
        pltpu.VMEM((chips, rows, cols), bf16),
        pltpu.VMEM((chips, rows, cols), bf16),
        pltpu.VMEM((chips, rows, cols), bf16),
        pltpu.VMEM((chips, rows, cols), bf16),
        pltpu.VMEM((2, 8, rows), f32),
        pltpu.VMEM((2, tp_count - 1, 8, rows), f32),
        pltpu.VMEM((rows, cols), f32),
        pltpu.VMEM((rows, cols), f32),
        pltpu.SemaphoreType.DMA((7,)),
        pltpu.SemaphoreType.DMA((copies,)),
        pltpu.SemaphoreType.DMA((copies,)),
    ]
    out = jax.ShapeDtypeStruct((rows, cols), bf16)
    first, second = pl.pallas_call(
        functools.partial(fused_kernel, (ep_count, tp_count, capacity, seq_length)),
        out_shape=(out, out),
        in_specs=[vmem] * 4 + [hbm] + [vmem] * 5
        + [hbm] * 6
        + [vmem, vmem],
        out_specs=(vmem, vmem),
        scratch_shapes=scratch,
        compiler_params=pltpu.CompilerParams(
            collective_id=0, has_side_effects=True, vmem_limit_bytes=VMEM_BYTES
        ),
    )(
        outer_gate,
        inner_gate,
        conv_value,
        conv_taps,
        mix_out,
        gain_mixer,
        bias_mixer,
        moe_input,
        route_ids.T,
        route_weights.T,
        expert_gate,
        expert_up,
        expert_down,
        shared_gate,
        shared_up,
        shared_down,
        gain_experts,
        bias_experts,
    )
    return pl.pallas_call(
        pass_kernel, out_shape=(out, out), in_specs=[vmem, vmem], out_specs=(vmem, vmem)
    )(first, second)


def on_device(*arrays):
    local_experts = arrays[10].shape[0]
    square = lax.axis_size("tp") == PLANE * PLANE
    if square and local_experts == 1 and lax.axis_size("ep") % CORES == 0:
        return fused_device(*arrays)
    return plain_device(*arrays)


def solution(mesh):
    in_specs = (
        P("ep", "tp"),
        P("ep", "tp"),
        P("ep", "tp"),
        P(None, "tp"),
        P(None, "tp"),
        P("tp"),
        P("tp"),
        P("ep", None),
        P("ep", None),
        P("ep", None),
        P("ep", None, "tp"),
        P("ep", None, "tp"),
        P("ep", None, "tp"),
        P(None, "tp"),
        P(None, "tp"),
        P(None, "tp"),
        P("tp"),
        P("tp"),
    )
    out_specs = (P("ep", "tp"), P("ep", "tp"))
    return jax.shard_map(
        on_device, mesh=mesh, in_specs=in_specs, out_specs=out_specs, check_vma=False
    )
```
